32 devices in a mesh: tp: 8 (over z, x), dp: 4 (over y, core).
Axes of the slice: x: 2, y: 2, z: 4, core: 2. Of those that a mesh axis runs over, the one named last changes fastest.
Arguments:
- stream: bfloat16 [128, 4096], P(None, 'dp'), may hold values from -12 to 12
- history: int32 [128], P('dp'), may hold values from 1 to 4096, 131072 in all
- input_norm_gain: float32 [2, 4096], P(None, 'dp'), may hold values from 0.1 to 1.9
- query_weight: bfloat16 [2, 4096, 4096], P(None, 'dp', 'tp'), may hold values from -0.09375 to 0.09375
- key_weight: bfloat16 [2, 4096, 4096], P(None, 'dp', 'tp'), may hold values from -0.09375 to 0.09375
- value_weight: bfloat16 [2, 4096, 4096], P(None, 'dp', 'tp'), may hold values from -0.09375 to 0.09375
- gate_weight: bfloat16 [2, 4096, 4096], P(None, 'dp', 'tp'), may hold values from -0.09375 to 0.09375
- adapter_down_weight: bfloat16 [2, 4096, 128], P(None, 'dp'), may hold values from -0.09375 to 0.09375
- decay_up_weight: float32 [2, 64, 4096], P(None, None, 'tp'), may hold values from -3 to 3
- rate_up_weight: float32 [2, 64, 4096], P(None, None, 'tp'), may hold values from -3 to 3
- decay_offset: float32 [2, 4096], P(None, 'tp'), may hold values from -3 to 1
- head_norm_gain: float32 [2, 4096], P(None, 'tp'), may hold values from 0.1 to 1.9
- output_weight: bfloat16 [2, 4096, 4096], P(None, 'tp', 'dp'), may hold values from -0.09375 to 0.09375
- recurrent_state: float32 [2, 128, 64, 4096], P(None, 'dp', 'tp'), may hold values from -5 to 5
Outputs:
- stream_out: bfloat16 [128, 4096], P(None, 'dp')
- state_out: float32 [2, 128, 64, 4096], P(None, 'dp', 'tp')
The draws below stay inside these ranges and needn't reach their ends.
All inputs are finite; a program needn't handle non-finite values. No bound on the sum of `history` on one device may be relied on, other than what follows from the above.
Results may differ from the reference program's by a relative error of at most 0.024.
Values may be sent and summed in bfloat16 or wider, within the bound.
No kernel may reach another device: no remote copies, remote signals or barrier semaphores. Data moves between devices by JAX's collectives and lax.ppermute only.
A program may use at most 128 MiB of HBM per device.

```python
import math
import jax
import jax.numpy as jnp
import numpy as np
from jax import lax

MODEL_WIDTH = 4096
HEAD = 64
ADAPTER_RANK = 64
SPAN = 64
BLOCK_COUNT = 2
BATCH = 128
HEADS = 64
N_DP = 4


def draw_stream(key, part):
    first_key, second_key = jax.random.split(jax.random.fold_in(key, 11))
    blocks = 8
    base = jax.random.normal(first_key, (BATCH, MODEL_WIDTH), jnp.float32)
    scales = jnp.exp(jax.random.uniform(second_key, (blocks,), jnp.float32, -1.1, 1.1))
    scales = jnp.repeat(scales, MODEL_WIDTH // blocks)
    return jnp.clip(base * scales[None, :], -12.0, 12.0).astype(jnp.bfloat16)


def level_of(own_key, extent, cuts, low, high):
    def one(position, shards_of):
        draws = jax.random.uniform(jax.random.fold_in(jax.random.fold_in(own_key, 6), position), (shards_of,), jnp.float32, low / len(cuts), high / len(cuts))
        return jnp.repeat(jnp.exp(draws), extent[position] // shards_of).reshape((-1,) + (1,) * (len(extent) - position - 1))

    loudness = one(*cuts[0])
    for cut in cuts[1:]:
        loudness = loudness * one(*cut)
    return loudness


def length_profile(count, total, limit, lean):
    loads = [(1 << 20) // math.isqrt(grade ** lean) + 1 for grade in range(2, count + 1)]
    spare, counts = total - limit - (count - 1), [1] * (count - 1)
    while spare > 0:
        candidates = [i for i in range(count - 1) if counts[i] < limit]
        mass, remaining = sum([loads[i] for i in candidates]), spare
        for i in candidates:
            more = min(limit - counts[i], max(1, remaining * loads[i] // mass), spare)
            counts[i] = counts[i] + more
            spare = spare - more
    return np.array([limit] + counts)


def ragged_sizes(stream_key, count, total, reach, slope):
    if count == 2:
        one = jax.random.randint(stream_key, (), max(1, total - reach), min(reach, total - 1) + 1)
        return jnp.stack([one, total - one])
    lengths = jnp.asarray(length_profile(count, total, reach, slope), jnp.int32)
    pairs = (count - 1) // 2
    donor, taker = lengths[1:1 + 2 * pairs:2], lengths[2:2 + 2 * pairs:2]
    room = jnp.minimum(donor - 1, reach - taker)
    shifted = jax.random.randint(jax.random.fold_in(stream_key, 1), (pairs,), 0, 1 << 20) % (room + 1)
    lengths = lengths.at[1:1 + 2 * pairs:2].set(donor - shifted).at[2:2 + 2 * pairs:2].set(taker + shifted)
    return lengths[jax.random.permutation(jax.random.fold_in(stream_key, 2), count)]


def gaussian(own_key, extent, scale, bound, pieces=(), dtype=jnp.bfloat16):
    entries = scale * jax.random.normal(own_key, extent, jnp.float32)
    if pieces:
        entries = entries * level_of(own_key, extent, pieces, -0.22, 0.18)
    return jnp.clip(entries, -bound, bound).astype(dtype)


def setup_inputs(seed: int = 0) -> dict:
    streams_of = jax.random.split(jax.random.key(seed), 15)
    stream = draw_stream(jax.random.fold_in(streams_of[14], 71), 0)
    history = ragged_sizes(streams_of[1], BATCH, 1024 * BATCH, 4096, 2).astype(jnp.int32)
    input_norm_gain = jnp.clip(1.0 + 0.18 * jax.random.normal(streams_of[2], (BLOCK_COUNT, MODEL_WIDTH), jnp.float32), 0.1, 1.9)
    query_weight = gaussian(streams_of[3], (BLOCK_COUNT, MODEL_WIDTH, MODEL_WIDTH), MODEL_WIDTH ** -0.5, 0.09375, ((1, 4), (2, 8)))
    key_weight = gaussian(streams_of[4], (BLOCK_COUNT, MODEL_WIDTH, MODEL_WIDTH), MODEL_WIDTH ** -0.5, 0.09375, ((1, 4), (2, 8)))
    value_weight = gaussian(streams_of[5], (BLOCK_COUNT, MODEL_WIDTH, MODEL_WIDTH), MODEL_WIDTH ** -0.5, 0.09375, ((1, 4), (2, 8)))
    gate_weight = gaussian(streams_of[6], (BLOCK_COUNT, MODEL_WIDTH, MODEL_WIDTH), MODEL_WIDTH ** -0.5, 0.09375, ((1, 4), (2, 8)))
    adapter_down_weight = gaussian(streams_of[7], (BLOCK_COUNT, MODEL_WIDTH, 2 * ADAPTER_RANK), MODEL_WIDTH ** -0.5, 0.09375, ((1, 4),))
    decay_up_weight = gaussian(streams_of[8], (BLOCK_COUNT, ADAPTER_RANK, MODEL_WIDTH), (ADAPTER_RANK // 16) ** -0.5, 3.0, ((2, 8),), jnp.float32)
    rate_up_weight = gaussian(streams_of[9], (BLOCK_COUNT, ADAPTER_RANK, MODEL_WIDTH), (ADAPTER_RANK // 16) ** -0.5, 3.0, ((2, 8),), jnp.float32)
    decay_offset = jnp.clip(-3.0 + 4.0 * jax.random.uniform(streams_of[10], (BLOCK_COUNT, MODEL_WIDTH), jnp.float32) ** level_of(streams_of[10], (BLOCK_COUNT, MODEL_WIDTH), ((1, 8),), -0.2, 0.2), -3.0, 1.0)
    head_norm_gain = jnp.clip(1.0 + 0.18 * jax.random.normal(streams_of[11], (BLOCK_COUNT, MODEL_WIDTH), jnp.float32), 0.1, 1.9)
    output_weight = gaussian(streams_of[12], (BLOCK_COUNT, MODEL_WIDTH, MODEL_WIDTH), MODEL_WIDTH ** -0.5, 0.09375, ((1, 8), (2, 4)))
    recurrent_state = gaussian(streams_of[13], (BLOCK_COUNT, BATCH, HEADS, HEAD * HEAD), 1.0, 5.0, ((1, 4), (2, 8)), jnp.float32)
    return {"stream": stream, "history": history, "input_norm_gain": input_norm_gain, "query_weight": query_weight, "key_weight": key_weight, "value_weight": value_weight, "gate_weight": gate_weight, "adapter_down_weight": adapter_down_weight, "decay_up_weight": decay_up_weight, "rate_up_weight": rate_up_weight, "decay_offset": decay_offset, "head_norm_gain": head_norm_gain, "output_weight": output_weight, "recurrent_state": recurrent_state}


NORM_EPS = 0.25
GROUP_EPS = 0.25

def projected_rows(rescaled_rows, weight):
    batch_rows = rescaled_rows.shape[0]
    blocked = rescaled_rows.reshape(batch_rows, N_DP, MODEL_WIDTH // N_DP).astype(jnp.float32)
    weight_blocks = weight.reshape(N_DP, MODEL_WIDTH // N_DP, weight.shape[1]).astype(jnp.float32)
    partials = jnp.einsum('bnd,ndc->nbc', blocked, weight_blocks)
    rounded = lax.optimization_barrier(partials.astype(jnp.bfloat16))
    return lax.optimization_barrier(jnp.sum(rounded.astype(jnp.float32), axis=0))

def mixing_block(stream, history, input_norm_gain, query_weight, key_weight, value_weight, gate_weight, adapter_down_weight, decay_up_weight, rate_up_weight, decay_offset, head_norm_gain, output_weight, recurrent_state):
    widened = stream.astype(jnp.float32)
    squares = lax.optimization_barrier(jnp.sum(widened * widened, axis=1))
    inverse_root_mean = lax.rsqrt(squares / MODEL_WIDTH + NORM_EPS)[:, None]
    rescaled_rows = (widened * input_norm_gain[None, :]).astype(jnp.bfloat16)
    query = projected_rows(rescaled_rows, query_weight) * inverse_root_mean
    key_proj = projected_rows(rescaled_rows, key_weight) * inverse_root_mean
    value_proj = projected_rows(rescaled_rows, value_weight) * inverse_root_mean
    gate_pre = projected_rows(rescaled_rows, gate_weight) * inverse_root_mean
    adapter_hidden = projected_rows(rescaled_rows, adapter_down_weight) * inverse_root_mean
    pos_factor = 0.5 + (history // SPAN % 3).astype(jnp.float32)
    decay_logits = decay_offset[None, :] + jnp.dot(jnp.tanh(adapter_hidden[:, :ADAPTER_RANK]), decay_up_weight, precision=lax.Precision.HIGHEST)
    rate_log = -jax.nn.softplus(-decay_logits) - 0.5
    decay = jnp.exp(-jnp.exp(rate_log) * pos_factor[:, None])
    learning_rate = jax.nn.sigmoid(jnp.dot(adapter_hidden[:, ADAPTER_RANK:], rate_up_weight, precision=lax.Precision.HIGHEST))
    batch_rows = widened.shape[0]
    head_count = MODEL_WIDTH // HEAD

    def heads_of(values):
        return values.reshape(batch_rows, head_count, HEAD)
    keys = heads_of(key_proj)
    key_unit = keys * lax.rsqrt(lax.optimization_barrier(jnp.sum(keys * keys, axis=-1, keepdims=True)) + 1.0)
    key_rate = key_unit * heads_of(learning_rate)
    matrix = recurrent_state.reshape(batch_rows, head_count, HEAD, HEAD)
    state_key = jnp.einsum('bhvk,bhk->bhv', matrix, key_unit)
    refreshed_state = matrix * heads_of(decay)[:, :, None, :] - state_key[..., None] * key_rate[:, :, None, :] + heads_of(value_proj)[..., None] * keys[:, :, None, :]
    readout = jnp.einsum('bhvk,bhk->bhv', refreshed_state, heads_of(query))
    mean_y = lax.optimization_barrier(jnp.mean(readout, axis=-1, keepdims=True))
    spread = lax.optimization_barrier(jnp.mean(jnp.square(readout - mean_y), axis=-1, keepdims=True))
    normed = ((readout - mean_y) * lax.rsqrt(spread + GROUP_EPS)).reshape(batch_rows, MODEL_WIDTH) * head_norm_gain[None, :]
    mixed = (normed * jax.nn.sigmoid(gate_pre)).astype(jnp.bfloat16)
    out_sum = jnp.dot(mixed, output_weight, preferred_element_type=jnp.float32)
    return ((widened + out_sum).astype(jnp.bfloat16), refreshed_state.reshape(batch_rows, head_count, HEAD * HEAD))

def reference(stream, history, input_norm_gain, query_weight, key_weight, value_weight, gate_weight, adapter_down_weight, decay_up_weight, rate_up_weight, decay_offset, head_norm_gain, output_weight, recurrent_state):
    new_states = []
    for layer_lookup in range(BLOCK_COUNT):
        stream, refreshed_state = mixing_block(stream, history, input_norm_gain[layer_lookup], query_weight[layer_lookup], key_weight[layer_lookup], value_weight[layer_lookup], gate_weight[layer_lookup], adapter_down_weight[layer_lookup], decay_up_weight[layer_lookup], rate_up_weight[layer_lookup], decay_offset[layer_lookup], head_norm_gain[layer_lookup], output_weight[layer_lookup], recurrent_state[layer_lookup])
        new_states.append(refreshed_state)
    return (stream, jnp.stack(new_states))
```

```python
import functools

import jax
import jax.numpy as jnp
from jax import lax
from jax.experimental import pallas as pl
from jax.experimental.pallas import tpu as pltpu
from jax.sharding import PartitionSpec as P

HEAD = 64
LANES = 128
SPAN = 64
NORM_EPS = 0.25
GROUP_EPS = 0.25
F32 = jnp.float32
BF16 = jnp.bfloat16


def project_kernel(x_ref, gain_ref, q_ref, k_ref, v_ref, g_ref, a_ref, out_ref, acc_ref, sq_ref):
    step = pl.program_id(0)
    last = pl.num_programs(0) - 1
    wide = x_ref[...].astype(F32)
    rows = (wide * gain_ref[0]).astype(BF16)

    @pl.when(step == 0)
    def _():
        acc_ref[...] = jnp.zeros_like(acc_ref)
        sq_ref[...] = jnp.zeros_like(sq_ref)

    sq_ref[...] += jnp.broadcast_to(jnp.sum(wide * wide, axis=1, keepdims=True), sq_ref.shape)
    at = 0
    for w_ref in (q_ref, k_ref, v_ref, g_ref, a_ref):
        cols = w_ref.shape[2]
        acc_ref[:, at : at + cols] += jnp.dot(rows, w_ref[0], preferred_element_type=F32)
        at += cols

    @pl.when(step == last)
    def _():
        out_ref[:, :at] = acc_ref[...].astype(BF16)
        squares = sq_ref[...]
        high = squares.astype(BF16)
        rest = squares - high.astype(F32)
        mid = rest.astype(BF16)
        low = (rest - mid.astype(F32)).astype(BF16)
        lane = lax.broadcasted_iota(jnp.int32, squares.shape, 1)
        packed = jnp.where(lane == 0, high.astype(F32), 0.0)
        packed = jnp.where(lane == 1, mid.astype(F32), packed)
        packed = jnp.where(lane == 2, low.astype(F32), packed)
        out_ref[:, at:] = packed.astype(BF16)


def project(layer, stream, gain, weights):
    batch, depth = stream.shape
    steps = 4
    part = depth // steps
    total = sum(w.shape[2] for w in weights)
    return pl.pallas_call(
        project_kernel,
        grid=(steps,),
        in_specs=[
            pl.BlockSpec((batch, part), lambda i: (0, i)),
            pl.BlockSpec((1, 1, part), lambda i: (layer, 0, i)),
        ]
        + [pl.BlockSpec((1, part, w.shape[2]), lambda i: (layer, i, 0)) for w in weights],
        out_specs=pl.BlockSpec((batch, total + LANES), lambda i: (0, 0)),
        out_shape=jax.ShapeDtypeStruct((batch, total + LANES), BF16),
        scratch_shapes=[pltpu.VMEM((batch, total), F32), pltpu.VMEM((batch, LANES), F32)],
        name=f"project_{layer}",
    )(stream, gain, *weights)


def recur_kernel(
    depth,
    width,
    block_seqs,
    recv_ref,
    pos_ref,
    decay_up_ref,
    rate_up_ref,
    offset_ref,
    hgain_ref,
    state_ref,
    *rest,
):
    mixed_ref, new_ref, q_s, k_s, ku_s, kr_s, d_s, v_s, gate_s, read_s = rest[-10:]
    heads = width // HEAD
    seqs = recv_ref.shape[1]
    step = pl.program_id(0)
    lane = lax.broadcasted_iota(jnp.int32, (1, LANES), 1)
    first = lane < HEAD

    @pl.when(step == 0)
    def _():
        total = recv_ref[0].astype(F32)
        for i in range(1, recv_ref.shape[0]):
            total = total + recv_ref[i].astype(F32)
        at = 4 * width + LANES
        squares = jnp.sum(total[:, at : at + LANES], axis=1, keepdims=True)
        inv = lax.rsqrt(squares / depth + NORM_EPS)
        hidden = total[:, 4 * width : at] * inv
        rank = LANES // 2
        tan = jnp.tanh(hidden[:, :rank])
        logits = offset_ref[0] + jnp.dot(
            tan, decay_up_ref[0], precision=lax.Precision.HIGHEST, preferred_element_type=F32
        )
        soft = jnp.maximum(-logits, 0.0) + jnp.log1p(jnp.exp(-jnp.abs(logits)))
        decay = jnp.exp(-jnp.exp(-soft - 0.5) * pos_ref[...])
        rate = jnp.dot(
            hidden[:, rank:], rate_up_ref[0], precision=lax.Precision.HIGHEST, preferred_element_type=F32
        )
        learn = 1.0 / (1.0 + jnp.exp(-rate))
        gate = total[:, 3 * width : 4 * width] * inv
        gate_s[...] = hgain_ref[0] / (1.0 + jnp.exp(-gate))
        for pair in range(width // LANES):
            for ref, values, base in (
                (q_s, total, 0),
                (k_s, total, width),
                (v_s, total, 2 * width),
                (d_s, decay, None),
                (kr_s, learn, None),
            ):
                lo = (base or 0) + pair * LANES
                x = values[:, lo : lo + LANES]
                if base is not None:
                    x = x * inv
                swapped = pltpu.roll(x, HEAD, 1)
                ref[pl.ds(2 * pair, seqs, stride=heads), :] = jnp.where(first, x, swapped)
                ref[pl.ds(2 * pair + 1, seqs, stride=heads), :] = jnp.where(first, swapped, x)
        keys = k_s[...]
        norm = 0.5 * jnp.sum(keys * keys, axis=1, keepdims=True)
        unit = keys * lax.rsqrt(norm + 1.0)
        ku_s[...] = unit
        kr_s[...] = unit * kr_s[...]

    rows = block_seqs * heads
    own = pl.ds(pl.multiple_of(step * rows, 8), rows)

    def twice(x):
        return jnp.concatenate([x, x], axis=1)

    query, keys, unit, key_rate, decay, value = (
        twice(r[own, :]) for r in (q_s, k_s, ku_s, kr_s, d_s, v_s)
    )
    wide = 2 * LANES
    ones = (
        lax.broadcasted_iota(jnp.int32, (wide, wide), 0) // HEAD
        == lax.broadcasted_iota(jnp.int32, (wide, wide), 1) // HEAD
    ).astype(F32).astype(BF16)
    wlane = lax.broadcasted_iota(jnp.int32, (1, wide), 1)
    group = wlane // HEAD
    within = wlane % HEAD
    readout = jnp.zeros((rows, wide), F32)

    def spread(x):
        return jnp.dot(x.astype(BF16), ones, preferred_element_type=F32)

    for t in range(HEAD * HEAD // wide):
        here = within == 4 * t + group
        old = state_ref[0, :, t * wide : (t + 1) * wide]
        state_key = spread(old * unit)
        values = spread(jnp.where(here, value, 0.0))
        new = old * decay - state_key * key_rate + values * keys
        new_ref[0, :, t * wide : (t + 1) * wide] = new
        readout = jnp.where(here, spread(new * query), readout)
    both = readout[:, :LANES] + readout[:, LANES:]
    both = both + pltpu.roll(both, HEAD, 1)
    mean = jnp.sum(both, axis=1, keepdims=True) / LANES
    centred = both - mean
    var = jnp.sum(centred * centred, axis=1, keepdims=True) / LANES
    read_s[...] = centred * lax.rsqrt(var + GROUP_EPS)
    mine = pl.ds(pl.multiple_of(step * block_seqs, 8), block_seqs)
    for pair in range(width // LANES):
        even = read_s[pl.ds(2 * pair, block_seqs, stride=heads), :]
        odd = read_s[pl.ds(2 * pair + 1, block_seqs, stride=heads), :]
        lanes = slice(pair * LANES, (pair + 1) * LANES)
        mixed_ref[:, lanes] = (jnp.where(first, even, odd) * gate_s[mine, lanes]).astype(BF16)


def recur(layer, depth, received, pos, decay_up, rate_up, offset, head_gain, state, earlier):
    parts, seqs, cols = received.shape
    layers, rows, per_head = state.shape
    width = decay_up.shape[2]
    heads = width // HEAD
    block_seqs = 8
    steps = seqs // block_seqs
    block_rows = block_seqs * heads
    rank = decay_up.shape[1]
    in_specs = [
        pl.BlockSpec((parts, seqs, cols), lambda i: (0, 0, 0)),
        pl.BlockSpec((seqs, 1), lambda i: (0, 0)),
        pl.BlockSpec((1, rank, width), lambda i: (layer, 0, 0)),
        pl.BlockSpec((1, rank, width), lambda i: (layer, 0, 0)),
        pl.BlockSpec((1, 1, width), lambda i: (layer, 0, 0)),
        pl.BlockSpec((1, 1, width), lambda i: (layer, 0, 0)),
        pl.BlockSpec((1, block_rows, per_head), lambda i: (layer, i, 0)),
    ]
    args = [received, pos, decay_up, rate_up, offset, head_gain, state]
    aliases = {}
    if earlier is not None:
        aliases = {len(args): 1}
        in_specs.append(pl.BlockSpec(memory_space=pl.ANY))
        args.append(earlier)
    tall = pltpu.VMEM((rows, LANES), F32)
    return pl.pallas_call(
        functools.partial(recur_kernel, depth, width, block_seqs),
        grid=(steps,),
        in_specs=in_specs,
        out_specs=(
            pl.BlockSpec((block_seqs, width), lambda i: (i, 0)),
            pl.BlockSpec((1, block_rows, per_head), lambda i: (layer, i, 0)),
        ),
        out_shape=(
            jax.ShapeDtypeStruct((seqs, width), BF16),
            jax.ShapeDtypeStruct(state.shape, F32),
        ),
        scratch_shapes=[tall] * 6
        + [pltpu.VMEM((seqs, width), F32), pltpu.VMEM((block_rows, LANES), F32)],
        input_output_aliases=aliases,
        name=f"recur_{layer}",
    )(*args)


def make_body(n_tp, n_dp):
    def body(
        stream,
        history,
        input_norm_gain,
        query_weight,
        key_weight,
        value_weight,
        gate_weight,
        adapter_down_weight,
        decay_up_weight,
        rate_up_weight,
        decay_offset,
        head_norm_gain,
        output_weight,
        recurrent_state,
    ):
        batch, depth_local = stream.shape
        seqs = history.shape[0]
        layers = input_norm_gain.shape[0]
        shape = recurrent_state.shape
        state = recurrent_state.reshape(layers, shape[1] * shape[2], shape[3])
        pos = (0.5 + (history // SPAN % 3).astype(F32))[:, None]
        weights = (query_weight, key_weight, value_weight, gate_weight, adapter_down_weight)
        own_rows = batch // n_tp
        own = lax.dynamic_slice_in_dim(stream, lax.axis_index("tp") * own_rows, own_rows, 0)
        new_state = None
        for layer in range(layers):
            packed = project(layer, stream, input_norm_gain[:, None, :], weights)
            received = lax.all_to_all(packed, "dp", 0, 0, tiled=True)
            mixed, new_state = recur(
                layer,
                depth_local * n_dp,
                received.reshape(n_dp, seqs, -1),
                pos,
                decay_up_weight,
                rate_up_weight,
                decay_offset[:, None, :],
                head_norm_gain[:, None, :],
                state,
                new_state,
            )
            terms = jnp.dot(
                lax.all_gather(mixed, "dp", axis=0, tiled=True),
                output_weight[layer],
                preferred_element_type=F32,
            ).astype(BF16)
            swapped = lax.all_to_all(terms, "tp", 0, 0, tiled=True)
            total = jnp.sum(swapped.reshape(n_tp, own_rows, depth_local).astype(F32), axis=0)
            own = (own.astype(F32) + total).astype(BF16)
            stream = lax.all_gather(own, "tp", axis=0, tiled=True)
        return stream, new_state.reshape(shape)

    return body


def solution(mesh):
    placed = (
        P(None, "dp"),
        P("dp"),
        P(None, "dp"),
        P(None, "dp", "tp"),
        P(None, "dp", "tp"),
        P(None, "dp", "tp"),
        P(None, "dp", "tp"),
        P(None, "dp", None),
        P(None, None, "tp"),
        P(None, None, "tp"),
        P(None, "tp"),
        P(None, "tp"),
        P(None, "tp", "dp"),
        P(None, "dp", "tp", None),
    )
    return jax.shard_map(
        make_body(mesh.shape["tp"], mesh.shape["dp"]),
        mesh=mesh,
        in_specs=placed,
        out_specs=(P(None, "dp"), P(None, "dp", "tp", None)),
        check_vma=False,
    )
```

```python
import functools

import jax
import jax.numpy as jnp
from jax import lax
from jax.experimental import pallas as pl
from jax.experimental.pallas import tpu as pltpu
from jax.sharding import PartitionSpec as P

HEAD = 64
LANES = 128
SPAN = 64
NORM_EPS = 0.25
GROUP_EPS = 0.25
F32 = jnp.float32
BF16 = jnp.bfloat16


def project_kernel(n_in, steps, idx_ref, *refs):
    x_refs = refs[:n_in]
    gain_ref, q_ref, k_ref, v_ref, g_ref, a_ref = refs[n_in : n_in + 6]
    outs = refs[n_in + 6 : -3]
    x_s, acc_ref, sq_ref = refs[-3:]
    step = pl.program_id(0)
    part = gain_ref.shape[2]

    @pl.when(step == 0)
    def _():
        acc_ref[...] = jnp.zeros_like(acc_ref)
        sq_ref[...] = jnp.zeros_like(sq_ref)
        rows = x_refs[0].shape[0]
        for d, x_ref in enumerate(x_refs):
            at = pl.multiple_of(lax.rem(idx_ref[0] + (n_in - d), n_in) * rows, 8)
            for s in range(steps):
                x_s[s, pl.ds(at, rows), :] = x_ref[:, s * part : (s + 1) * part].astype(F32)

    wide = x_s[step]
    rows = (wide * gain_ref[0]).astype(BF16)
    sq_ref[...] += jnp.broadcast_to(jnp.sum(wide * wide, axis=1, keepdims=True), sq_ref.shape)
    at = 0
    for w_ref in (q_ref, k_ref, v_ref, g_ref, a_ref):
        cols = w_ref.shape[2]
        acc_ref[:, at : at + cols] += jnp.dot(rows, w_ref[0], preferred_element_type=F32)
        at += cols

    @pl.when(step == steps - 1)
    def _():
        squares = sq_ref[...]
        high = squares.astype(BF16).astype(F32)
        mid = (squares - high).astype(BF16).astype(F32)
        low = (squares - high - mid).astype(BF16).astype(F32)
        core = lax.rem(idx_ref[1], 2)
        chip = lax.div(idx_ref[1], 2)
        half = len(outs) // 2
        lane = lax.broadcasted_iota(jnp.int32, squares.shape, 1) - 3 * core
        packed = jnp.where(lane == 0, high, 0.0)
        packed = jnp.where(lane == 1, mid, packed)
        acc_ref[:, at:] = jnp.where(lane == 2, low, packed)
        seqs = outs[0].shape[0]
        for e in range(half):
            base = 2 * lax.rem(chip + e, half)
            for out, which in ((outs[e], core), (outs[half + e], 1 - core)):
                row = pl.multiple_of((base + which) * seqs, 8)
                out[...] = acc_ref[pl.ds(row, seqs), :].astype(BF16)


def project(layer, idx, blocks, gain, weights, n_dp):
    depth = gain.shape[2]
    batch = sum(b.shape[0] for b in blocks)
    seqs = batch // n_dp
    steps = 4
    part = depth // steps
    total = sum(w.shape[2] for w in weights) + LANES
    outs = n_dp
    return pl.pallas_call(
        functools.partial(project_kernel, len(blocks), steps),
        grid=(steps,),
        in_specs=[pl.BlockSpec(memory_space=pltpu.SMEM)]
        + [pl.BlockSpec(b.shape, lambda i: (0, 0)) for b in blocks]
        + [pl.BlockSpec((1, 1, part), lambda i: (layer, 0, i))]
        + [pl.BlockSpec((1, part, w.shape[2]), lambda i: (layer, i, 0)) for w in weights],
        out_specs=[pl.BlockSpec((seqs, total), lambda i: (0, 0))] * outs,
        out_shape=[jax.ShapeDtypeStruct((seqs, total), BF16)] * outs,
        scratch_shapes=[
            pltpu.VMEM((steps, batch, part), F32),
            pltpu.VMEM((batch, total), F32),
            pltpu.VMEM((batch, LANES), F32),
        ],
        name=f"project_{layer}",
    )(idx, *blocks, gain, *weights)


def twice(x):
    return jnp.concatenate([x, x], axis=1)


def spreader():
    wide = 2 * LANES
    ones = (
        lax.broadcasted_iota(jnp.int32, (wide, wide), 0) // HEAD
        == lax.broadcasted_iota(jnp.int32, (wide, wide), 1) // HEAD
    ).astype(F32).astype(BF16)
    wlane = lax.broadcasted_iota(jnp.int32, (1, wide), 1)
    return lambda x: jnp.dot(x.astype(BF16), ones, preferred_element_type=F32), wlane // HEAD, wlane % HEAD


def recur_kernel(n_in, depth, width, block_seqs, *refs):
    recv = refs[:n_in]
    pos_ref, decay_up_ref, rate_up_ref, offset_ref, hgain_ref, state_ref = refs[n_in : n_in + 6]
    mixed_ref, k_s, kr_s, d_s, v_s, sk_s = refs[n_in + 6 : n_in + 12]
    ku_s, dq_s, q_s, gate_s, read_s = refs[n_in + 12 :]
    heads = width // HEAD
    seqs = recv[0].shape[0]
    step = pl.program_id(0)
    lane = lax.broadcasted_iota(jnp.int32, (1, LANES), 1)
    first = lane < HEAD

    @pl.when(step == 0)
    def _():
        total = recv[0][...].astype(F32)
        for r in recv[1:]:
            total = total + r[...].astype(F32)
        at = 4 * width + LANES
        squares = jnp.sum(total[:, at : at + LANES], axis=1, keepdims=True)
        inv = lax.rsqrt(squares / depth + NORM_EPS)
        hidden = total[:, 4 * width : at] * inv
        rank = LANES // 2
        tan = jnp.tanh(hidden[:, :rank])
        logits = offset_ref[0] + jnp.dot(
            tan, decay_up_ref[0], precision=lax.Precision.HIGHEST, preferred_element_type=F32
        )
        soft = jnp.maximum(-logits, 0.0) + jnp.log1p(jnp.exp(-jnp.abs(logits)))
        decay = jnp.exp(-jnp.exp(-soft - 0.5) * pos_ref[...])
        rate = jnp.dot(
            hidden[:, rank:], rate_up_ref[0], precision=lax.Precision.HIGHEST, preferred_element_type=F32
        )
        learn = 1.0 / (1.0 + jnp.exp(-rate))
        gate = total[:, 3 * width : 4 * width] * inv
        gate_s[...] = hgain_ref[0] / (1.0 + jnp.exp(-gate))
        for pair in range(width // LANES):
            for ref, values, base in (
                (q_s, total, 0),
                (k_s, total, width),
                (v_s, total, 2 * width),
                (d_s, decay, None),
                (kr_s, learn, None),
            ):
                lo = (base or 0) + pair * LANES
                x = values[:, lo : lo + LANES]
                if base is not None:
                    x = x * inv
                swapped = pltpu.roll(x, HEAD, 1)
                ref[pl.ds(2 * pair, seqs, stride=heads), :] = jnp.where(first, x, swapped)
                ref[pl.ds(2 * pair + 1, seqs, stride=heads), :] = jnp.where(first, swapped, x)
        keys = k_s[...]
        norm = 0.5 * jnp.sum(keys * keys, axis=1, keepdims=True)
        unit = keys * lax.rsqrt(norm + 1.0)
        ku_s[...] = unit
        kr_s[...] = unit * kr_s[...]
        dq_s[...] = d_s[...] * q_s[...]

    rows = block_seqs * heads
    own = pl.ds(pl.multiple_of(step * rows, 8), rows)
    unit, faded = twice(ku_s[own, :]), twice(dq_s[own, :])
    wide = 2 * LANES
    spread, group, within = spreader()
    readout = jnp.zeros((rows, wide), F32)
    matched = jnp.zeros((rows, wide), F32)
    for t in range(HEAD * HEAD // wide):
        here = within == 4 * t + group
        old = state_ref[0, :, t * wide : (t + 1) * wide]
        matched = jnp.where(here, spread(old * unit), matched)
        readout = jnp.where(here, spread(old * faded), readout)

    def folded(x):
        x = x[:, :LANES] + x[:, LANES:]
        return x + pltpu.roll(x, HEAD, 1)

    matched = folded(matched)
    sk_s[own, :] = matched
    query = q_s[own, :]
    along_rate = 0.5 * jnp.sum(kr_s[own, :] * query, axis=1, keepdims=True)
    along_key = 0.5 * jnp.sum(k_s[own, :] * query, axis=1, keepdims=True)
    both = folded(readout) - matched * along_rate + v_s[own, :] * along_key
    mean = jnp.sum(both, axis=1, keepdims=True) / LANES
    centred = both - mean
    var = jnp.sum(centred * centred, axis=1, keepdims=True) / LANES
    read_s[...] = centred * lax.rsqrt(var + GROUP_EPS)
    mine = pl.ds(pl.multiple_of(step * block_seqs, 8), block_seqs)
    for pair in range(width // LANES):
        even = read_s[pl.ds(2 * pair, block_seqs, stride=heads), :]
        odd = read_s[pl.ds(2 * pair + 1, block_seqs, stride=heads), :]
        lanes = slice(pair * LANES, (pair + 1) * LANES)
        mixed_ref[:, lanes] = (jnp.where(first, even, odd) * gate_s[mine, lanes]).astype(BF16)


def recur(layer, depth, received, pos, decay_up, rate_up, offset, head_gain, state):
    seqs, cols = received[0].shape
    layers, rows, per_head = state.shape
    width = decay_up.shape[2]
    heads = width // HEAD
    block_seqs = 8
    block_rows = block_seqs * heads
    rank = decay_up.shape[1]
    tall = (rows, LANES)
    return pl.pallas_call(
        functools.partial(recur_kernel, len(received), depth, width, block_seqs),
        grid=(seqs // block_seqs,),
        in_specs=[pl.BlockSpec((seqs, cols), lambda i: (0, 0))] * len(received)
        + [
            pl.BlockSpec((seqs, 1), lambda i: (0, 0)),
            pl.BlockSpec((1, rank, width), lambda i: (layer, 0, 0)),
            pl.BlockSpec((1, rank, width), lambda i: (layer, 0, 0)),
            pl.BlockSpec((1, 1, width), lambda i: (layer, 0, 0)),
            pl.BlockSpec((1, 1, width), lambda i: (layer, 0, 0)),
            pl.BlockSpec((1, block_rows, per_head), lambda i: (layer, i, 0)),
        ],
        out_specs=[pl.BlockSpec((block_seqs, width), lambda i: (i, 0))]
        + [pl.BlockSpec(tall, lambda i: (0, 0))] * 5,
        out_shape=[jax.ShapeDtypeStruct((seqs, width), BF16)]
        + [jax.ShapeDtypeStruct(tall, F32)] * 5,
        scratch_shapes=[pltpu.VMEM(tall, F32)] * 3
        + [pltpu.VMEM((seqs, width), F32), pltpu.VMEM((block_rows, LANES), F32)],
        name=f"recur_{layer}",
    )(*received, pos, decay_up, rate_up, offset, head_gain, state)


def update_kernel(k_ref, kr_ref, d_ref, v_ref, sk_ref, state_ref, *rest):
    new_ref = rest[-1]
    keys, key_rate, decay, value, matched = (
        twice(r[...]) for r in (k_ref, kr_ref, d_ref, v_ref, sk_ref)
    )
    wide = 2 * LANES
    spread, group, within = spreader()
    for t in range(HEAD * HEAD // wide):
        here = within == 4 * t + group
        old = state_ref[0, :, t * wide : (t + 1) * wide]
        state_key = spread(jnp.where(here, matched, 0.0))
        values = spread(jnp.where(here, value, 0.0))
        new_ref[0, :, t * wide : (t + 1) * wide] = old * decay - state_key * key_rate + values * keys


def update(layer, coefficients, state, after, earlier):
    layers, rows, per_head = state.shape
    block_rows = min(64, rows)
    args = [*coefficients, state, after]
    in_specs = [pl.BlockSpec((block_rows, LANES), lambda i: (i, 0))] * 5 + [
        pl.BlockSpec((1, block_rows, per_head), lambda i: (layer, i, 0)),
        pl.BlockSpec(memory_space=pl.ANY),
    ]
    aliases = {}
    if earlier is not None:
        aliases = {len(args): 0}
        in_specs.append(pl.BlockSpec(memory_space=pl.ANY))
        args.append(earlier)
    return pl.pallas_call(
        update_kernel,
        grid=(rows // block_rows,),
        in_specs=in_specs,
        out_specs=pl.BlockSpec((1, block_rows, per_head), lambda i: (layer, i, 0)),
        out_shape=jax.ShapeDtypeStruct(state.shape, F32),
        input_output_aliases=aliases,
        name=f"update_{layer}",
    )(*args)


def output_kernel(n_in, idx_ref, *refs):
    blocks = refs[:n_in]
    w_ref = refs[n_in]
    outs = refs[n_in + 1 : -2]
    x_s, y_s = refs[-2:]
    rows = blocks[0].shape[0]
    for d, block in enumerate(blocks):
        at = pl.multiple_of(lax.rem(idx_ref[1] + (n_in - d), n_in) * rows, 8)
        x_s[pl.ds(at, rows), :] = block[...].astype(F32)
    y_s[...] = jnp.dot(x_s[...].astype(BF16), w_ref[0], preferred_element_type=F32)
    part = outs[0].shape[0]
    for d, out in enumerate(outs):
        at = pl.multiple_of(lax.rem(idx_ref[0] + d, len(outs)) * part, 8)
        out[...] = y_s[pl.ds(at, part), :].astype(BF16)


def output(layer, idx, blocks, weight, n_tp):
    seqs, width = blocks[0].shape
    batch = seqs * len(blocks)
    cols = weight.shape[2]
    part = batch // n_tp
    whole = pl.BlockSpec((seqs, width), lambda i: (0, 0))
    return pl.pallas_call(
        functools.partial(output_kernel, len(blocks)),
        grid=(1,),
        in_specs=[pl.BlockSpec(memory_space=pltpu.SMEM)]
        + [whole] * len(blocks)
        + [pl.BlockSpec((1, width, cols), lambda i: (layer, 0, 0))],
        out_specs=[pl.BlockSpec((part, cols), lambda i: (0, 0))] * n_tp,
        out_shape=[jax.ShapeDtypeStruct((part, cols), BF16)] * n_tp,
        scratch_shapes=[pltpu.VMEM((batch, width), F32), pltpu.VMEM((batch, cols), F32)],
        name=f"output_{layer}",
    )(idx, *blocks, weight)


def place_kernel(n_in, idx_ref, *refs):
    out_ref, x_s = refs[-2:]
    rows = refs[0].shape[0]
    for d in range(n_in):
        at = pl.multiple_of(lax.rem(idx_ref[0] + (n_in - d), n_in) * rows, 8)
        x_s[pl.ds(at, rows), :] = refs[d][...].astype(F32)
    out_ref[...] = x_s[...].astype(BF16)


def place(idx, blocks):
    rows, cols = blocks[0].shape
    batch = rows * len(blocks)
    return pl.pallas_call(
        functools.partial(place_kernel, len(blocks)),
        grid=(1,),
        in_specs=[pl.BlockSpec(memory_space=pltpu.SMEM)]
        + [pl.BlockSpec((rows, cols), lambda i: (0, 0))] * len(blocks),
        out_specs=pl.BlockSpec((batch, cols), lambda i: (0, 0)),
        out_shape=jax.ShapeDtypeStruct((batch, cols), BF16),
        scratch_shapes=[pltpu.VMEM((batch, cols), F32)],
        name="place",
    )(idx, *blocks)


def turn(n, d):
    return [(i, (i + d) % n) for i in range(n)]


def gather_blocks(x, axis, n):
    return [x] + [lax.ppermute(x, axis, turn(n, d)) for d in range(1, n)]


def swap_blocks(blocks, axis):
    n = len(blocks)
    return blocks[:1] + [lax.ppermute(blocks[d], axis, turn(n, d)) for d in range(1, n)]


def make_body(n_tp, n_dp):
    def body(
        stream,
        history,
        input_norm_gain,
        query_weight,
        key_weight,
        value_weight,
        gate_weight,
        adapter_down_weight,
        decay_up_weight,
        rate_up_weight,
        decay_offset,
        head_norm_gain,
        output_weight,
        recurrent_state,
    ):
        batch, depth_local = stream.shape
        layers = input_norm_gain.shape[0]
        shape = recurrent_state.shape
        state = recurrent_state.reshape(layers, shape[1] * shape[2], shape[3])
        pos = (0.5 + (history // SPAN % 3).astype(F32))[:, None]
        weights = (query_weight, key_weight, value_weight, gate_weight, adapter_down_weight)
        idx = jnp.stack([lax.axis_index("tp"), lax.axis_index("dp")]).astype(jnp.int32)
        own_rows = batch // n_tp
        own = lax.dynamic_slice_in_dim(stream, lax.axis_index("tp") * own_rows, own_rows, 0)
        half = n_dp // 2
        partner = [(i, i ^ 1) for i in range(n_dp)]
        blocks = [stream]
        new_state = None
        for layer in range(layers):
            parts = list(project(layer, idx, blocks, input_norm_gain[:, None, :], weights, n_dp))
            kept, given = parts[:half], parts[half:]
            taken = [None] * half
            for e in list(range(1, half)) + [0]:
                taken[e] = lax.ppermute(given[e], "dp", partner)
            received = [kept[0], taken[0]]
            for e in range(1, half):
                pair_sum = (kept[e].astype(F32) + taken[e].astype(F32)).astype(BF16)
                route = [(i, (i // 2 + e) % half * 2 + i % 2) for i in range(n_dp)]
                received.append(lax.ppermute(pair_sum, "dp", route))
            mixed, *coefficients = recur(
                layer,
                depth_local * n_dp,
                received,
                pos,
                decay_up_weight,
                rate_up_weight,
                decay_offset[:, None, :],
                head_norm_gain[:, None, :],
                state,
            )
            terms = list(output(layer, idx, gather_blocks(mixed, "dp", n_dp), output_weight, n_tp))
            swapped = swap_blocks(terms, "tp")
            new_state = update(layer, coefficients, state, terms[0], new_state)
            swapped, new_state = lax.optimization_barrier((swapped, new_state))
            total = own.astype(F32)
            for block in swapped:
                total = total + block.astype(F32)
            own = total.astype(BF16)
            blocks = gather_blocks(own, "tp", n_tp)
        return place(idx, blocks), new_state.reshape(shape)

    return body


def solution(mesh):
    placed = (
        P(None, "dp"),
        P("dp"),
        P(None, "dp"),
        P(None, "dp", "tp"),
        P(None, "dp", "tp"),
        P(None, "dp", "tp"),
        P(None, "dp", "tp"),
        P(None, "dp", None),
        P(None, None, "tp"),
        P(None, None, "tp"),
        P(None, "tp"),
        P(None, "tp"),
        P(None, "tp", "dp"),
        P(None, "dp", "tp", None),
    )
    return jax.shard_map(
        make_body(mesh.shape["tp"], mesh.shape["dp"]),
        mesh=mesh,
        in_specs=placed,
        out_specs=(P(None, "dp"), P(None, "dp", "tp", None)),
        check_vma=False,
    )
```
